1024 devices in a mesh: rep: 4 (over z_hi), fs: 32 (over z_lo, y), tp: 8 (over x, core).
Axes of the slice: x: 4, y: 4, z: 32 (z_hi: 4, z_lo: 8; z = z_hi * 8 + z_lo), core: 2. Of those that a mesh axis runs over, the one named last changes fastest.
Arguments:
- tokens: bfloat16 [128, 768, 2048], P(('rep', 'fs')), may hold values from -6 to 6
- norm_gain: float32 [2048], replicated, may hold values from 0.1 to 1.9
- outer_weight: bfloat16 [2048, 2048], P('fs', 'tp'), may hold values from -0.125 to 0.125
- inner_weight: bfloat16 [2048, 2048], P('fs', 'tp'), may hold values from -0.125 to 0.125
- value_weight: bfloat16 [2048, 2048], P('fs', 'tp'), may hold values from -0.125 to 0.125
- conv_taps: float32 [3, 2048], replicated, may hold values from -3.5 to 3.5
- out_weight: bfloat16 [2048, 2048], P('fs', 'tp'), may hold values from -0.125 to 0.125
Outputs:
- mixed: bfloat16 [128, 768, 2048], P(('rep', 'fs'), None, 'tp')
The draws below stay inside these ranges and needn't reach their ends.
All inputs are finite; a program needn't handle non-finite values.
Results may differ from the reference program's by a relative error of at most 0.014.
Values may be sent and summed in bfloat16 or wider, within the bound.
No kernel may reach another device: no remote copies, remote signals or barrier semaphores. Data moves between devices by JAX's collectives and lax.ppermute only.
A program may use at most 32 MiB of HBM per device.

```python
import jax
import jax.numpy as jnp
from jax import lax

D = 2048
TAPS = 3
SEQ = 768
BATCH = 128


def steps_of(rng, dims, cuts, least, top_value):
    level = 1.0
    for axis_at, parts in cuts:
        heights = jax.random.uniform(jax.random.fold_in(jax.random.fold_in(rng, 6), axis_at), (parts,), jnp.float32, least / len(cuts), top_value / len(cuts))
        level = level * jnp.repeat(jnp.exp(heights), dims[axis_at] // parts).reshape((-1,) + (1,) * (len(dims) - 1 - axis_at))
    return level


def bell_draw(key, extent, deviation, limit, cuts=(), kind=jnp.bfloat16):
    array = deviation * jax.random.normal(key, extent, jnp.float32)
    if cuts:
        array = array * steps_of(key, extent, cuts, -0.22, 0.18)
    return jnp.clip(array, -limit, limit).astype(kind)


def setup_inputs(seed: int = 0) -> dict:
    seeds = jax.random.split(jax.random.key(seed), 8)
    tokens = bell_draw(seeds[0], (BATCH, SEQ, D), 1.0, 6.0, ((0, 128),))
    norm_gain = jnp.clip(1.0 + 0.18 * jax.random.normal(seeds[1], (D,), jnp.float32), 0.1, 1.9)
    outer_weight = bell_draw(seeds[2], (D, D), D ** -0.5, 0.125, ((0, 32), (1, 8)))
    inner_weight = bell_draw(seeds[3], (D, D), D ** -0.5, 0.125, ((0, 32), (1, 8)))
    value_weight = bell_draw(seeds[4], (D, D), D ** -0.5, 0.125, ((0, 32), (1, 8)))
    conv_taps = bell_draw(seeds[5], (TAPS, D), TAPS ** -0.5, 3.5, (), jnp.float32)
    out_weight = bell_draw(seeds[6], (D, D), D ** -0.5, 0.125, ((0, 32), (1, 8)))
    return {"tokens": tokens, "norm_gain": norm_gain, "outer_weight": outer_weight, "inner_weight": inner_weight, "value_weight": value_weight, "conv_taps": conv_taps, "out_weight": out_weight}


def reference(tokens, norm_gain, outer_weight, inner_weight, value_weight, conv_taps, out_weight):
    xf = tokens.astype(jnp.float32)
    scale = lax.rsqrt(lax.optimization_barrier(jnp.mean(xf * xf, axis=-1, keepdims=True)) + 1e-06)
    normed = (xf * scale * norm_gain).astype(jnp.bfloat16)
    rows = normed.reshape(BATCH * SEQ, D)
    outer = jnp.dot(rows, outer_weight, preferred_element_type=jnp.float32).astype(jnp.bfloat16)
    inner = jnp.dot(rows, inner_weight, preferred_element_type=jnp.float32).astype(jnp.bfloat16)
    value = jnp.dot(rows, value_weight, preferred_element_type=jnp.float32).astype(jnp.bfloat16)
    product = (inner.astype(jnp.float32) * value.astype(jnp.float32)).reshape(BATCH, SEQ, D)
    padded = jnp.pad(product, ((0, 0), (TAPS - 1, 0), (0, 0)))
    convolved = jnp.zeros((BATCH, SEQ, D), jnp.float32)
    for k in range(TAPS):
        convolved = convolved + conv_taps[k] * padded[:, k:k + SEQ, :]
    gated = (outer.astype(jnp.float32) * convolved.reshape(BATCH * SEQ, D)).astype(jnp.bfloat16)
    total = jnp.dot(gated, out_weight, preferred_element_type=jnp.float32)
    return total.astype(jnp.bfloat16).reshape(BATCH, SEQ, D)
```

```python
import functools

import jax
import jax.numpy as jnp
from jax import lax
from jax.experimental import pallas as pl
from jax.experimental.pallas import tpu as pltpu
from jax.sharding import Mesh
from jax.sharding import PartitionSpec as P


LINE = ("rep", "z")


def ring(size, step):
    return [(i, (i + step) % size) for i in range(size)]


def shift(x, axis, step):
    names = (axis,) if isinstance(axis, str) else axis
    size = 1
    for name in names:
        size *= lax.axis_size(name)
    return lax.ppermute(x, axis, ring(size, step))


def to_peers(x, axis):
    peers = lax.axis_size(axis)
    return lax.all_to_all(jnp.broadcast_to(x[None], (peers, *x.shape)), axis, 0, 0, tiled=True)


def norm_kernel(x_ref, gain_ref, out_ref):
    rows = 64
    gain = gain_ref[...]

    def step(i, _):
        at = pl.ds(pl.multiple_of(i * rows, rows), rows)
        x = x_ref[at, :].astype(jnp.float32)
        scale = lax.rsqrt(jnp.mean(x * x, axis=-1, keepdims=True) + 1e-06)
        out_ref[at, :] = (x * scale * gain).astype(jnp.bfloat16)
        return 0

    lax.fori_loop(0, x_ref.shape[0] // rows, step, 0)


def gate_kernel(at_ref, normed_ref, near_ref, far_ref, taps_ref, out_ref, weight, product):
    z = at_ref[0]
    columns = out_ref.shape[1]
    seq = out_ref.shape[0]
    for offset in range(8):
        block = lax.rem(z + offset + 4, 8)
        at = pl.ds(pl.multiple_of(block * 256, 256), 256)
        if 3 <= offset <= 5:
            piece = near_ref[:, offset - 3]
        else:
            piece = far_ref[:, offset if offset < 3 else offset - 3]
        weight[at, :] = piece.reshape(256, 3 * columns)
    product[0:8, :] = jnp.zeros((8, columns), jnp.float32)
    rows = 256
    for r in range(0, seq, rows):
        normed = normed_ref[r : r + rows, :]

        def project(k, normed=normed):
            w = weight[:, k * columns : (k + 1) * columns]
            return jnp.dot(normed, w, preferred_element_type=jnp.float32).astype(jnp.bfloat16)

        inner = project(1).astype(jnp.float32)
        value = project(2).astype(jnp.float32)
        product[8 + r : 8 + r + rows, :] = inner * value
        outer = project(0).astype(jnp.float32)
        convolved = taps_ref[0:1, :] * product[6 + r : 6 + r + rows, :]
        convolved = convolved + taps_ref[1:2, :] * product[7 + r : 7 + r + rows, :]
        convolved = convolved + taps_ref[2:3, :] * product[8 + r : 8 + r + rows, :]
        out_ref[r : r + rows, :] = (outer * convolved).astype(jnp.bfloat16)


def out_kernel(at_ref, *refs):
    gated, all_ref, out_ref, weight = refs[:8], refs[8], refs[9], refs[10]
    z, x, core = at_ref[0], at_ref[1], at_ref[2]
    seq = out_ref.shape[0]
    for side in range(2):
        for k, step in enumerate((0, -1, 1, 2)):
            tile = 2 * lax.rem(x + step + 4, 4) + lax.rem(core + side, 2)
            offset = lax.rem(tile - z + 12, 8)
            at = (side * 4 + k) * 256
            weight[at : at + 256, :] = all_ref[:, offset].reshape(256, out_ref.shape[1])
    rows = 256
    for r in range(0, seq, rows):
        left = jnp.concatenate([g[r : r + rows, :] for g in gated], axis=1)
        total = jnp.dot(left, weight[...], preferred_element_type=jnp.float32)
        out_ref[r : r + rows, :] = total.astype(jnp.bfloat16)


VMEM = pl.BlockSpec(memory_space=pltpu.VMEM)
SMEM = pl.BlockSpec(memory_space=pltpu.SMEM)


def cost(flops, moved):
    return pl.CostEstimate(flops=flops, bytes_accessed=moved, transcendentals=0)


def gather_z(block):
    behind = shift(block, LINE, 1)
    ahead = shift(block, LINE, -1)
    near = jnp.stack([behind, block, ahead])
    low = shift(near, LINE, 3)
    high = shift(near[:2], LINE, -3)
    return near, low, high


def local(tokens, norm_gain, outer_weight, inner_weight, value_weight, conv_taps, out_weight):
    seq, width = tokens.shape[1:]
    columns = outer_weight.shape[1]
    z, x, core = lax.axis_index("z"), lax.axis_index("x"), lax.axis_index("core")
    place = jnp.stack([z, x, core]).astype(jnp.int32)

    block = jnp.concatenate([outer_weight, inner_weight, value_weight], axis=1)
    near, low, high = gather_z(block)
    near_all = to_peers(near, "y")
    normed = pl.pallas_call(
        norm_kernel,
        out_shape=jax.ShapeDtypeStruct((seq, width), jnp.bfloat16),
        in_specs=[VMEM, VMEM],
        out_specs=VMEM,
        name="norm",
        cost_estimate=cost(8 * seq * width, 4 * seq * width),
    )(tokens.reshape(seq, width), norm_gain.reshape(1, width))
    far_all = to_peers(jnp.concatenate([low, high]), "y")

    out_near, out_low, out_high = gather_z(out_weight)
    with jax.named_scope("rows_y"):
        out_all = to_peers(jnp.concatenate([out_low, out_near, out_high]), "y")

    offset = (2 * x + core) * columns
    taps = lax.dynamic_slice_in_dim(conv_taps, offset, columns, 1)
    gated = pl.pallas_call(
        gate_kernel,
        out_shape=jax.ShapeDtypeStruct((seq, columns), jnp.bfloat16),
        in_specs=[SMEM, VMEM, VMEM, VMEM, VMEM],
        out_specs=VMEM,
        scratch_shapes=[
            pltpu.VMEM((width, 3 * columns), jnp.bfloat16),
            pltpu.VMEM((8 + seq, columns), jnp.float32),
        ],
        name="gate",
        cost_estimate=cost(6 * seq * width * columns, 8 * seq * width),
    )(place, normed, near_all, far_all, taps)

    swap = [(0, 1), (1, 0)]
    own = [gated] + [shift(gated, "x", step) for step in (1, -1, 2)]
    other = [lax.ppermute(g, "core", swap) for g in own]
    result = pl.pallas_call(
        out_kernel,
        out_shape=jax.ShapeDtypeStruct((seq, columns), jnp.bfloat16),
        in_specs=[SMEM] + [VMEM] * 9,
        out_specs=VMEM,
        scratch_shapes=[pltpu.VMEM((width, columns), jnp.bfloat16)],
        name="project",
        cost_estimate=cost(2 * seq * width * columns, 4 * seq * width),
    )(place, *own, *other, out_all)
    return result.reshape(1, seq, columns)


def solution(mesh):
    devices = mesh.devices.reshape(4, 8, 4, 4, 2)
    fine = Mesh(devices, ("rep", "z", "y", "x", "core"))
    fs, tp = ("z", "y"), ("x", "core")
    in_specs = (
        P(("rep", "z", "y"), None, None),
        P(),
        P(fs, tp),
        P(fs, tp),
        P(fs, tp),
        P(),
        P(fs, tp),
    )
    out_specs = P(("rep", "z", "y"), None, tp)
    return jax.shard_map(local, mesh=fine, in_specs=in_specs, out_specs=out_specs, check_vma=False)
```

```python
import jax
import jax.numpy as jnp
from jax import lax
from jax.experimental import pallas as pl
from jax.experimental.pallas import tpu as pltpu
from jax.sharding import Mesh
from jax.sharding import PartitionSpec as P


LINE = ("rep", "zh", "zl")


def ring(size, step):
    return [(i, (i + step) % size) for i in range(size)]


def size_of(axis):
    names = (axis,) if isinstance(axis, str) else axis
    size = 1
    for name in names:
        size *= lax.axis_size(name)
    return size


def shift(x, axis, step):
    return lax.ppermute(x, axis, ring(size_of(axis), step))


def mirror(x):
    size = size_of(LINE)
    return lax.ppermute(x, LINE, [(i, (i + (-1, -3, 3, 1)[i % 4]) % size) for i in range(size)])


def copies_of(x, axis):
    return jnp.broadcast_to(x[None], (lax.axis_size(axis), *x.shape))


def exchange(copies, axis):
    return lax.all_to_all(copies, axis, 0, 0, tiled=True)


def pack_kernel(outer_ref, inner_ref, value_ref, out_ref):
    packed = jnp.concatenate([outer_ref[...], inner_ref[...], value_ref[...]], axis=1)
    for p in range(out_ref.shape[0]):
        out_ref[p] = packed


def norm_kernel(x_ref, gain_ref, out_ref):
    rows = 64
    gain = gain_ref[...]

    def step(i, _):
        at = pl.ds(pl.multiple_of(i * rows, rows), rows)
        x = x_ref[at, :].astype(jnp.float32)
        scale = lax.rsqrt(jnp.mean(x * x, axis=-1, keepdims=True) + 1e-06)
        out_ref[at, :] = (x * scale * gain).astype(jnp.bfloat16)
        return 0

    lax.fori_loop(0, x_ref.shape[0] // rows, step, 0)


ROWS = 256


def half_dot(normed_ref, weight_ref, group, r):
    depth = 256 * weight_ref.shape[1]
    at = pl.ds(pl.multiple_of(group * depth, depth), depth)
    weight = [weight_ref[:, b].reshape(256, weight_ref.shape[3]) for b in range(weight_ref.shape[1])]
    return jnp.dot(
        normed_ref[r : r + ROWS, at],
        jnp.concatenate(weight, axis=0),
        preferred_element_type=jnp.float32,
    )


def near_kernel(at_ref, normed_ref, weight_ref, total_ref):
    for r in range(0, normed_ref.shape[0], ROWS):
        total_ref[r : r + ROWS, :] = half_dot(normed_ref, weight_ref, at_ref[0], r)


def gate_kernel(at_ref, normed_ref, weight_ref, total_ref, taps_ref, out_ref, product):
    seq, columns = out_ref.shape
    product[0:8, :] = jnp.zeros((8, columns), jnp.float32)
    for r in range(0, seq, ROWS):
        parts = total_ref[r : r + ROWS, :] + half_dot(normed_ref, weight_ref, 1 - at_ref[0], r)
        parts = parts.astype(jnp.bfloat16).astype(jnp.float32)
        outer, inner, value = (parts[:, k * columns : (k + 1) * columns] for k in range(3))
        product[8 + r : 8 + r + ROWS, :] = inner * value
        convolved = taps_ref[0:1, :] * product[6 + r : 6 + r + ROWS, :]
        convolved = convolved + taps_ref[1:2, :] * product[7 + r : 7 + r + ROWS, :]
        convolved = convolved + taps_ref[2:3, :] * product[8 + r : 8 + r + ROWS, :]
        out_ref[r : r + ROWS, :] = (outer * convolved).astype(jnp.bfloat16)


def out_kernel(at_ref, *refs):
    gated, all_ref, out_ref = refs[:8], refs[8], refs[9]
    z, x, core = at_ref[1], at_ref[2], at_ref[3]
    seq, columns = out_ref.shape
    pieces = []
    for side in range(2):
        for step in (0, -1, 1, 2):
            tile = 2 * lax.rem(x + step + 4, 4) + lax.rem(core + side, 2)
            offset = lax.rem(tile - z + 12, 8)
            pieces.append(all_ref[:, offset].reshape(256, columns))
    weight = jnp.concatenate(pieces, axis=0)
    for r in range(0, seq, ROWS):
        left = jnp.concatenate([g[r : r + ROWS, :] for g in gated], axis=1)
        total = jnp.dot(left, weight, preferred_element_type=jnp.float32)
        out_ref[r : r + ROWS, :] = total.astype(jnp.bfloat16)


VMEM = pl.BlockSpec(memory_space=pltpu.VMEM)
SMEM = pl.BlockSpec(memory_space=pltpu.SMEM)


def call(kernel, shape, dtype, in_specs, flops, moved, scratch=(), limit=24):
    return pl.pallas_call(
        kernel,
        out_shape=jax.ShapeDtypeStruct(shape, dtype),
        in_specs=in_specs,
        out_specs=VMEM,
        scratch_shapes=list(scratch),
        cost_estimate=pl.CostEstimate(flops=flops, bytes_accessed=moved, transcendentals=0),
        compiler_params=pltpu.CompilerParams(vmem_limit_bytes=limit << 20),
    )


def gather_z(block):
    behind = shift(block, LINE, 1)
    ahead = shift(block, LINE, -1)
    near = jnp.stack([behind, block, ahead])
    low = shift(near, LINE, 3)
    high = shift(near[:2], LINE, -3)
    return jnp.concatenate([low, near, high])


def local(tokens, norm_gain, outer_weight, inner_weight, value_weight, conv_taps, out_weight):
    seq, width = tokens.shape[1:]
    depth, columns = outer_weight.shape
    bf16, f32 = jnp.bfloat16, jnp.float32
    half = lax.axis_index("zh")
    z = half * lax.axis_size("zl") + lax.axis_index("zl")
    x, core = lax.axis_index("x"), lax.axis_index("core")
    place = jnp.stack([half, z, x, core]).astype(jnp.int32)

    packed = call(pack_kernel, (4, depth, 3 * columns), bf16, [VMEM] * 3, 8 * depth * columns, 30 * depth * columns)
    group = exchange(packed(outer_weight, inner_weight, value_weight), "zl")
    other_group = mirror(group)
    near = exchange(copies_of(group, "y"), "y")

    norm = call(norm_kernel, (seq, width), bf16, [VMEM] * 2, 8 * seq * width, 4 * seq * width)
    normed = norm(tokens.reshape(seq, width), norm_gain.reshape(1, width))
    flops = 3 * seq * width * columns
    total = call(near_kernel, (seq, 3 * columns), f32, [SMEM] + [VMEM] * 2, flops, 8 * seq * width)(place, normed, near)
    far = exchange(copies_of(other_group, "y"), "y")

    out_rows = gather_z(out_weight)
    taps = lax.dynamic_slice_in_dim(conv_taps, (2 * x + core) * columns, columns, 1)
    gate = call(
        gate_kernel,
        (seq, columns),
        bf16,
        [SMEM] + [VMEM] * 4,
        flops,
        8 * seq * width,
        [pltpu.VMEM((8 + seq, columns), f32)],
    )
    gated = gate(place, normed, far, total, taps)

    own = [gated]
    for step in (1, -1, 2):
        own.append(shift(gated, "x", step))
    out_all = exchange(copies_of(out_rows, "y"), "y")
    other = [lax.ppermute(g, "core", [(0, 1), (1, 0)]) for g in own]
    project = call(out_kernel, (seq, columns), bf16, [SMEM] + [VMEM] * 9, 2 * seq * width * columns, 4 * seq * width)
    return project(place, *own, *other, out_all).reshape(1, seq, columns)


def solution(mesh):
    devices = mesh.devices.reshape(4, 2, 4, 4, 4, 2)
    fine = Mesh(devices, ("rep", "zh", "zl", "y", "x", "core"))
    fs, tp = ("zh", "zl", "y"), ("x", "core")
    in_specs = (
        P(("rep", *fs), None, None),
        P(),
        P(fs, tp),
        P(fs, tp),
        P(fs, tp),
        P(),
        P(fs, tp),
    )
    out_specs = P(("rep", *fs), None, tp)

    return jax.shard_map(local, mesh=fine, in_specs=in_specs, out_specs=out_specs, check_vma=False)
```

```python
import jax
import jax.numpy as jnp
from jax import lax
from jax.experimental import pallas as pl
from jax.experimental.pallas import tpu as pltpu
from jax.sharding import Mesh
from jax.sharding import PartitionSpec as P


LINE = ("rep", "zh", "zl")


def ring(size, step):
    return [(i, (i + step) % size) for i in range(size)]


def size_of(axis):
    names = (axis,) if isinstance(axis, str) else axis
    size = 1
    for name in names:
        size *= lax.axis_size(name)
    return size


def shift(x, axis, step):
    return lax.ppermute(x, axis, ring(size_of(axis), step))


def mirror(x):
    size = size_of(LINE)
    return lax.ppermute(x, LINE, [(i, (i + (-1, -3, 3, 1)[i % 4]) % size) for i in range(size)])


def exchange(copies, axis):
    return lax.all_to_all(copies, axis, 0, 0, tiled=True)


def pack_kernel(outer_ref, inner_ref, value_ref, out_ref, held, sems):
    copies = [
        pltpu.make_async_copy(ref, held.at[k], sems.at[k])
        for k, ref in enumerate((outer_ref, inner_ref, value_ref))
    ]
    for copy in copies:
        copy.start()
    columns = held.shape[2]
    for k, copy in enumerate(copies):
        copy.wait()
        for p in range(out_ref.shape[0]):
            out_ref[p, :, k * columns : (k + 1) * columns] = held[k]


def norm_kernel(x_ref, gain_ref, out_ref):
    rows = 64
    gain = gain_ref[...]

    def step(i, _):
        at = pl.ds(pl.multiple_of(i * rows, rows), rows)
        x = x_ref[at, :].astype(jnp.float32)
        scale = lax.rsqrt(jnp.mean(x * x, axis=-1, keepdims=True) + 1e-06)
        out_ref[at, :] = (x * scale * gain).astype(jnp.bfloat16)
        return 0

    lax.fori_loop(0, x_ref.shape[0] // rows, step, 0)


ROWS = 256
STEPS = (0, -1, 1, 2)


def place_rows(at_ref, pieces, weight):
    for piece, step in zip(pieces, STEPS):
        y = lax.rem(at_ref[4] + step + 4, 4)
        for b in range(piece.shape[0]):
            weight[pl.ds(pl.multiple_of(b * 256 + y * 64, 64), 64), :] = piece[b]


def half_dot(normed_ref, weight, group, r):
    depth = weight.shape[0]
    at = pl.ds(pl.multiple_of(group * depth, depth), depth)
    return jnp.dot(normed_ref[r : r + ROWS, at], weight[...], preferred_element_type=jnp.float32)


def near_kernel(at_ref, normed_ref, *refs):
    pieces, total_ref, weight = refs[:4], refs[4], refs[5]
    place_rows(at_ref, pieces, weight)
    for r in range(0, normed_ref.shape[0], ROWS):
        total_ref[r : r + ROWS, :] = half_dot(normed_ref, weight, at_ref[0], r)


def gate_kernel(at_ref, normed_ref, *refs):
    pieces, total_ref, taps_ref, out_ref, weight, product = refs[:4], *refs[4:]
    place_rows(at_ref, pieces, weight)
    seq, columns = out_ref.shape
    product[0:8, :] = jnp.zeros((8, columns), jnp.float32)
    for r in range(0, seq, ROWS):
        parts = total_ref[r : r + ROWS, :] + half_dot(normed_ref, weight, 1 - at_ref[0], r)
        parts = parts.astype(jnp.bfloat16).astype(jnp.float32)
        outer, inner, value = (parts[:, k * columns : (k + 1) * columns] for k in range(3))
        product[8 + r : 8 + r + ROWS, :] = inner * value
        convolved = taps_ref[0:1, :] * product[6 + r : 6 + r + ROWS, :]
        convolved = convolved + taps_ref[1:2, :] * product[7 + r : 7 + r + ROWS, :]
        convolved = convolved + taps_ref[2:3, :] * product[8 + r : 8 + r + ROWS, :]
        out_ref[r : r + ROWS, :] = (outer * convolved).astype(jnp.bfloat16)


def out_kernel(at_ref, *refs):
    gated, pieces, out_ref, weight = refs[:8], refs[8:12], refs[12], refs[13]
    z, x, core, y = at_ref[1], at_ref[2], at_ref[3], at_ref[4]
    for side in range(2):
        for k, step in enumerate(STEPS):
            tile = 2 * lax.rem(x + step + 4, 4) + lax.rem(core + side, 2)
            offset = lax.rem(tile - z + 12, 8)
            for piece, other in zip(pieces, STEPS):
                at = (side * 4 + k) * 256 + lax.rem(y + other + 4, 4) * 64
                weight[pl.ds(pl.multiple_of(at, 64), 64), :] = piece[offset]
    for r in range(0, out_ref.shape[0], ROWS):
        left = jnp.concatenate([g[r : r + ROWS, :] for g in gated], axis=1)
        total = jnp.dot(left, weight[...], preferred_element_type=jnp.float32)
        out_ref[r : r + ROWS, :] = total.astype(jnp.bfloat16)


VMEM = pl.BlockSpec(memory_space=pltpu.VMEM)
ANY = pl.BlockSpec(memory_space=pl.ANY)
SMEM = pl.BlockSpec(memory_space=pltpu.SMEM)


def call(kernel, shape, dtype, in_specs, flops, moved, scratch=(), limit=24):
    return pl.pallas_call(
        kernel,
        out_shape=jax.ShapeDtypeStruct(shape, dtype),
        in_specs=in_specs,
        out_specs=VMEM,
        scratch_shapes=list(scratch),
        cost_estimate=pl.CostEstimate(flops=flops, bytes_accessed=moved, transcendentals=0),
        compiler_params=pltpu.CompilerParams(vmem_limit_bytes=limit << 20),
    )


def pieces_of(x, axis):
    pieces = [x]
    for step in (1, -1, 2):
        pieces.append(shift(x, axis, step))
    return pieces


def gather_z(block):
    behind = shift(block, LINE, 1)
    ahead = shift(block, LINE, -1)
    near = jnp.stack([behind, block, ahead])
    low = shift(near, LINE, 3)
    high = shift(near[:2], LINE, -3)
    return jnp.concatenate([low, near, high])


def local(tokens, norm_gain, outer_weight, inner_weight, value_weight, conv_taps, out_weight):
    seq, width = tokens.shape[1:]
    depth, columns = outer_weight.shape
    bf16, f32 = jnp.bfloat16, jnp.float32
    half = lax.axis_index("zh")
    z = half * lax.axis_size("zl") + lax.axis_index("zl")
    x, core = lax.axis_index("x"), lax.axis_index("core")
    place = jnp.stack([half, z, x, core, lax.axis_index("y")]).astype(jnp.int32)

    packed = call(
        pack_kernel,
        (4, depth, 3 * columns),
        bf16,
        [ANY] * 3,
        8 * depth * columns,
        30 * depth * columns,
        [pltpu.VMEM((3, depth, columns), bf16), pltpu.SemaphoreType.DMA((3,))],
        limit=60,
    )
    group = exchange(packed(outer_weight, inner_weight, value_weight), "zl")
    other_group = mirror(group)
    near = pieces_of(group, "y")

    norm = call(norm_kernel, (seq, width), bf16, [VMEM] * 2, 8 * seq * width, 4 * seq * width)
    normed = norm(tokens.reshape(seq, width), norm_gain.reshape(1, width))
    flops = 3 * seq * width * columns
    weight = pltpu.VMEM((width // 2, 3 * columns), bf16)
    start = call(
        near_kernel, (seq, 3 * columns), f32, [SMEM] + [VMEM] * 5, flops, 8 * seq * width, [weight]
    )
    total = start(place, normed, *near)
    far = pieces_of(other_group, "y")

    out_rows = gather_z(out_weight)
    taps = lax.dynamic_slice_in_dim(conv_taps, (2 * x + core) * columns, columns, 1)
    gate = call(
        gate_kernel,
        (seq, columns),
        bf16,
        [SMEM] + [VMEM] * 7,
        flops,
        8 * seq * width,
        [weight, pltpu.VMEM((8 + seq, columns), f32)],
    )
    rows = pieces_of(out_rows, "y")
    gated = gate(place, normed, *far, total, taps)

    own = pieces_of(gated, "x")
    other = []
    for g in own:
        other.append(lax.ppermute(g, "core", [(0, 1), (1, 0)]))
    project = call(
        out_kernel,
        (seq, columns),
        bf16,
        [SMEM] + [VMEM] * 12,
        2 * seq * width * columns,
        4 * seq * width,
        [pltpu.VMEM((width, columns), bf16)],
    )
    return project(place, *own, *other, *rows).reshape(1, seq, columns)


def solution(mesh):
    devices = mesh.devices.reshape(4, 2, 4, 4, 4, 2)
    fine = Mesh(devices, ("rep", "zh", "zl", "y", "x", "core"))
    fs, tp = ("zh", "zl", "y"), ("x", "core")
    in_specs = (
        P(("rep", *fs), None, None),
        P(),
        P(fs, tp),
        P(fs, tp),
        P(fs, tp),
        P(),
        P(fs, tp),
    )
    out_specs = P(("rep", *fs), None, tp)

    return jax.shard_map(local, mesh=fine, in_specs=in_specs, out_specs=out_specs, check_vma=False)
```

```python
import jax
import jax.numpy as jnp
from jax import lax
from jax.experimental import pallas as pl
from jax.experimental.pallas import tpu as pltpu
from jax.sharding import Mesh
from jax.sharding import PartitionSpec as P


LINE = ("rep", "zh", "zl")


def ring(size, step):
    return [(i, (i + step) % size) for i in range(size)]


def size_of(axis):
    names = (axis,) if isinstance(axis, str) else axis
    size = 1
    for name in names:
        size *= lax.axis_size(name)
    return size


def shift(x, axis, step):
    return lax.ppermute(x, axis, ring(size_of(axis), step))


def mirror(x):
    size = size_of(LINE)
    return lax.ppermute(x, LINE, [(i, (i + (-1, -3, 3, 1)[i % 4]) % size) for i in range(size)])


def exchange(copies, axis):
    return lax.all_to_all(copies, axis, 0, 0, tiled=True)


def pack_kernel(outer_ref, inner_ref, value_ref, out_ref, held, sems):
    copies = [
        pltpu.make_async_copy(ref, held.at[k], sems.at[k])
        for k, ref in enumerate((outer_ref, inner_ref, value_ref))
    ]
    for copy in copies:
        copy.start()
    columns = held.shape[2]
    for k, copy in enumerate(copies):
        copy.wait()
        for p in range(out_ref.shape[0]):
            out_ref[p, :, k * columns : (k + 1) * columns] = held[k]


def norm_kernel(x_ref, gain_ref, out_ref, held, sems):
    rows = held.shape[1]
    chunks = x_ref.shape[0] // rows
    gain = gain_ref[...]
    small = 32

    def fetch(i):
        return pltpu.make_async_copy(x_ref.at[pl.ds(i * rows, rows)], held.at[i % 2], sems.at[i % 2])

    fetch(0).start()
    for i in range(chunks):
        if i + 1 < chunks:
            fetch(i + 1).start()
        fetch(i).wait()

        def step(j, _, i=i):
            at = pl.multiple_of(j * small, small)
            x = held[i % 2, pl.ds(at, small), :].astype(jnp.float32)
            scale = lax.rsqrt(jnp.mean(x * x, axis=-1, keepdims=True) + 1e-06)
            out_ref[pl.ds(i * rows + at, small), :] = (x * scale * gain).astype(jnp.bfloat16)
            return 0

        lax.fori_loop(0, rows // small, step, 0)


ROWS = 256
STEPS = (0, -1, 1, 2)


def place_rows(at_ref, pieces, weight):
    for piece, step in zip(pieces, STEPS):
        y = lax.rem(at_ref[4] + step + 4, 4)
        for b in range(piece.shape[0]):
            weight[pl.ds(pl.multiple_of(b * 256 + y * 64, 64), 64), :] = piece[b]


def half_dot(normed_ref, weight, group, r):
    depth = weight.shape[0]
    at = pl.ds(pl.multiple_of(group * depth, depth), depth)
    return jnp.dot(normed_ref[r : r + ROWS, at], weight[...], preferred_element_type=jnp.float32)


def near_kernel(at_ref, normed_ref, *refs):
    pieces, total_ref, weight = refs[:4], refs[4], refs[5]
    place_rows(at_ref, pieces, weight)
    for r in range(0, normed_ref.shape[0], ROWS):
        total_ref[r : r + ROWS, :] = half_dot(normed_ref, weight, at_ref[0], r)


def gate_kernel(at_ref, normed_ref, *refs):
    pieces, total_ref, taps_ref, out_ref, weight, product = refs[:4], *refs[4:]
    place_rows(at_ref, pieces, weight)
    seq, columns = out_ref.shape[1:]
    product[0:8, :] = jnp.zeros((8, columns), jnp.float32)
    for r in range(0, seq, ROWS):
        parts = total_ref[r : r + ROWS, :] + half_dot(normed_ref, weight, 1 - at_ref[0], r)
        parts = parts.astype(jnp.bfloat16).astype(jnp.float32)
        outer, inner, value = (parts[:, k * columns : (k + 1) * columns] for k in range(3))
        product[8 + r : 8 + r + ROWS, :] = inner * value
        convolved = taps_ref[0:1, :] * product[6 + r : 6 + r + ROWS, :]
        convolved = convolved + taps_ref[1:2, :] * product[7 + r : 7 + r + ROWS, :]
        convolved = convolved + taps_ref[2:3, :] * product[8 + r : 8 + r + ROWS, :]
        gated = (outer * convolved).astype(jnp.bfloat16)
        for p in range(out_ref.shape[0]):
            out_ref[p, r : r + ROWS, :] = gated


def side_dot(gated_ref, weight, r):
    left = jnp.concatenate([gated_ref[k, r : r + ROWS, :] for k in range(gated_ref.shape[0])], axis=1)
    return jnp.dot(left, weight, preferred_element_type=jnp.float32)


def own_kernel(at_ref, gated_ref, *refs):
    pieces, total_ref, rest_ref, weight = refs[:4], refs[4], refs[5], refs[6]
    z, core, y = at_ref[1], at_ref[3], at_ref[4]
    for side, target in enumerate((weight, rest_ref)):
        for k in range(gated_ref.shape[0]):
            offset = lax.rem(2 * k + lax.rem(core + side, 2) - z + 12, 8)
            for piece, step in zip(pieces, STEPS):
                at = k * 256 + lax.rem(y + step + 4, 4) * 64
                target[pl.ds(pl.multiple_of(at, 64), 64), :] = piece[offset]
    for r in range(0, total_ref.shape[0], ROWS):
        total_ref[r : r + ROWS, :] = side_dot(gated_ref, weight[...], r)


def other_kernel(gated_ref, rest_ref, total_ref, out_ref):
    for r in range(0, out_ref.shape[0], ROWS):
        total = total_ref[r : r + ROWS, :] + side_dot(gated_ref, rest_ref[...], r)
        out_ref[r : r + ROWS, :] = total.astype(jnp.bfloat16)


VMEM = pl.BlockSpec(memory_space=pltpu.VMEM)
HBM = pl.BlockSpec(memory_space=pltpu.HBM)
ANY = pl.BlockSpec(memory_space=pl.ANY)
SMEM = pl.BlockSpec(memory_space=pltpu.SMEM)


def call(kernel, shape, dtype, in_specs, flops, moved, scratch=(), limit=24):
    shapes = [jax.ShapeDtypeStruct(*pair) for pair in zip(shape, dtype)] if isinstance(dtype, tuple) else None
    return pl.pallas_call(
        kernel,
        out_shape=shapes or jax.ShapeDtypeStruct(shape, dtype),
        in_specs=in_specs,
        out_specs=[VMEM] * len(shapes) if shapes else VMEM,
        scratch_shapes=list(scratch),
        cost_estimate=pl.CostEstimate(flops=flops, bytes_accessed=moved, transcendentals=0),
        compiler_params=pltpu.CompilerParams(vmem_limit_bytes=limit << 20),
    )


def pieces_of(x, axis):
    pieces = [x]
    for step in (1, -1, 2):
        pieces.append(shift(x, axis, step))
    return pieces


def gather_z(block):
    behind = shift(block, LINE, 1)
    ahead = shift(block, LINE, -1)
    near = jnp.stack([behind, block, ahead])
    low = shift(near, LINE, 3)
    high = shift(near[:2], LINE, -3)
    return jnp.concatenate([low, near, high])


def local(tokens, norm_gain, outer_weight, inner_weight, value_weight, conv_taps, out_weight):
    seq, width = tokens.shape[1:]
    depth, columns = outer_weight.shape
    bf16, f32 = jnp.bfloat16, jnp.float32
    half = lax.axis_index("zh")
    z = half * lax.axis_size("zl") + lax.axis_index("zl")
    x, core = lax.axis_index("x"), lax.axis_index("core")
    place = jnp.stack([half, z, x, core, lax.axis_index("y")]).astype(jnp.int32)

    packed = call(
        pack_kernel,
        (4, depth, 3 * columns),
        bf16,
        [ANY] * 3,
        8 * depth * columns,
        30 * depth * columns,
        [pltpu.VMEM((3, depth, columns), bf16), pltpu.SemaphoreType.DMA((3,))],
        limit=60,
    )
    group = exchange(packed(outer_weight, inner_weight, value_weight), "zl")
    other_group = mirror(group)
    near = pieces_of(group, "y")

    norm = call(
        norm_kernel,
        (seq, width),
        bf16,
        [HBM, VMEM],
        8 * seq * width,
        4 * seq * width,
        [pltpu.VMEM((2, 192, width), bf16), pltpu.SemaphoreType.DMA((2,))],
        limit=9,
    )
    normed = norm(tokens.reshape(seq, width), norm_gain.reshape(1, width))
    flops = 3 * seq * width * columns
    weight = pltpu.VMEM((width // 2, 3 * columns), bf16)
    start = call(near_kernel, (seq, 3 * columns), f32, [SMEM] + [VMEM] * 5, flops, 8 * seq * width, [weight])
    total = start(place, normed, *near)
    far = pieces_of(other_group, "y")

    out_rows = gather_z(out_weight)
    taps = lax.dynamic_slice_in_dim(conv_taps, (2 * x + core) * columns, columns, 1)
    gate = call(
        gate_kernel,
        (lax.axis_size("x"), seq, columns),
        bf16,
        [SMEM] + [VMEM] * 7,
        flops,
        8 * seq * width,
        [weight, pltpu.VMEM((8 + seq, columns), f32)],
    )
    rows = pieces_of(out_rows, "y")
    gated = gate(place, normed, *far, total, taps)

    own = exchange(gated, "x")
    other = lax.ppermute(own, "core", [(0, 1), (1, 0)])
    flops = seq * width * columns
    first = call(
        own_kernel,
        ((seq, columns), (width // 2, columns)),
        (f32, bf16),
        [SMEM] + [VMEM] * 5,
        flops,
        4 * seq * width,
        [pltpu.VMEM((width // 2, columns), bf16)],
    )
    total, rest = first(place, own, *rows)
    last = call(other_kernel, (seq, columns), bf16, [VMEM] * 3, flops, 4 * seq * width)
    return last(other, rest, total).reshape(1, seq, columns)


def solution(mesh):
    devices = mesh.devices.reshape(4, 2, 4, 4, 4, 2)
    fine = Mesh(devices, ("rep", "zh", "zl", "y", "x", "core"))
    fs, tp = ("zh", "zl", "y"), ("x", "core")
    in_specs = (
        P(("rep", *fs), None, None),
        P(),
        P(fs, tp),
        P(fs, tp),
        P(fs, tp),
        P(),
        P(fs, tp),
    )
    out_specs = P(("rep", *fs), None, tp)

    return jax.shard_map(local, mesh=fine, in_specs=in_specs, out_specs=out_specs, check_vma=False)
```

```python
import jax
import jax.numpy as jnp
from jax import lax
from jax.experimental import pallas as pl
from jax.experimental.pallas import tpu as pltpu
from jax.sharding import Mesh
from jax.sharding import PartitionSpec as P


LINE = ("rep", "zh", "zl")


def ring(size, step):
    return [(i, (i + step) % size) for i in range(size)]


def size_of(axis):
    names = (axis,) if isinstance(axis, str) else axis
    size = 1
    for name in names:
        size *= lax.axis_size(name)
    return size


def shift(x, axis, step):
    return lax.ppermute(x, axis, ring(size_of(axis), step))


def mirror(x):
    size = size_of(LINE)
    return lax.ppermute(x, LINE, [(i, (i + (-1, -3, 3, 1)[i % 4]) % size) for i in range(size)])


def exchange(copies, axis):
    return lax.all_to_all(copies, axis, 0, 0, tiled=True)


def pack_kernel(outer_ref, inner_ref, value_ref, out_ref, held, sems):
    copies = [
        pltpu.make_async_copy(ref, held.at[k], sems.at[k])
        for k, ref in enumerate((outer_ref, inner_ref, value_ref))
    ]
    for copy in copies:
        copy.start()
    columns = held.shape[2]
    for k, copy in enumerate(copies):
        copy.wait()
        for p in range(out_ref.shape[0]):
            out_ref[p, :, k * columns : (k + 1) * columns] = held[k]


def norm_kernel(x_ref, gain_ref, out_ref):
    rows = 64
    gain = gain_ref[...]

    def step(i, _):
        at = pl.ds(pl.multiple_of(i * rows, rows), rows)
        x = x_ref[at, :].astype(jnp.float32)
        scale = lax.rsqrt(jnp.mean(x * x, axis=-1, keepdims=True) + 1e-06)
        out_ref[at, :] = (x * scale * gain).astype(jnp.bfloat16)
        return 0

    lax.fori_loop(0, x_ref.shape[0] // rows, step, 0)


ROWS = 256
STEPS = (0, -1, 1, 2)


def place_rows(at_ref, pieces, weight):
    for piece, step in zip(pieces, STEPS):
        y = lax.rem(at_ref[4] + step + 4, 4)
        for b in range(piece.shape[0]):
            weight[pl.ds(pl.multiple_of(b * 256 + y * 64, 64), 64), :] = piece[b]


def half_dot(normed_ref, weight, group, r):
    depth = weight.shape[0]
    at = pl.ds(pl.multiple_of(group * depth, depth), depth)
    return jnp.dot(normed_ref[r : r + ROWS, at], weight[...], preferred_element_type=jnp.float32)


def near_kernel(at_ref, normed_ref, *refs):
    pieces, total_ref, weight = refs[:4], refs[4], refs[5]
    place_rows(at_ref, pieces, weight)
    for r in range(0, normed_ref.shape[0], ROWS):
        total_ref[r : r + ROWS, :] = half_dot(normed_ref, weight, at_ref[0], r)


def gate_kernel(at_ref, normed_ref, *refs):
    pieces, total_ref, taps_ref, out_ref, weight, product = refs[:4], *refs[4:]
    place_rows(at_ref, pieces, weight)
    seq, columns = out_ref.shape[1:]
    product[0:8, :] = jnp.zeros((8, columns), jnp.float32)
    for r in range(0, seq, ROWS):
        parts = total_ref[r : r + ROWS, :] + half_dot(normed_ref, weight, 1 - at_ref[0], r)
        parts = parts.astype(jnp.bfloat16).astype(jnp.float32)
        outer, inner, value = (parts[:, k * columns : (k + 1) * columns] for k in range(3))
        product[8 + r : 8 + r + ROWS, :] = inner * value
        convolved = taps_ref[0:1, :] * product[6 + r : 6 + r + ROWS, :]
        convolved = convolved + taps_ref[1:2, :] * product[7 + r : 7 + r + ROWS, :]
        convolved = convolved + taps_ref[2:3, :] * product[8 + r : 8 + r + ROWS, :]
        gated = (outer * convolved).astype(jnp.bfloat16)
        for p in range(out_ref.shape[0]):
            out_ref[p, r : r + ROWS, :] = gated


def side_dot(gated_ref, weight, r):
    left = jnp.concatenate([gated_ref[k, r : r + ROWS, :] for k in range(gated_ref.shape[0])], axis=1)
    return jnp.dot(left, weight, preferred_element_type=jnp.float32)


def own_kernel(at_ref, gated_ref, *refs):
    pieces, total_ref, rest_ref, weight = refs[:4], refs[4], refs[5], refs[6]
    z, core, y = at_ref[1], at_ref[3], at_ref[4]
    for side, target in enumerate((weight, rest_ref)):
        for k in range(gated_ref.shape[0]):
            offset = lax.rem(2 * k + lax.rem(core + side, 2) - z + 12, 8)
            for piece, step in zip(pieces, STEPS):
                at = k * 256 + lax.rem(y + step + 4, 4) * 64
                target[pl.ds(pl.multiple_of(at, 64), 64), :] = piece[offset]
    for r in range(0, total_ref.shape[0], ROWS):
        total_ref[r : r + ROWS, :] = side_dot(gated_ref, weight[...], r)


def other_kernel(gated_ref, rest_ref, total_ref, out_ref):
    for r in range(0, out_ref.shape[0], ROWS):
        total = total_ref[r : r + ROWS, :] + side_dot(gated_ref, rest_ref[...], r)
        out_ref[r : r + ROWS, :] = total.astype(jnp.bfloat16)


VMEM = pl.BlockSpec(memory_space=pltpu.VMEM)
ANY = pl.BlockSpec(memory_space=pl.ANY)
SMEM = pl.BlockSpec(memory_space=pltpu.SMEM)


def call(kernel, shape, dtype, in_specs, flops, moved, scratch=(), limit=24):
    shapes = [jax.ShapeDtypeStruct(*pair) for pair in zip(shape, dtype)] if isinstance(dtype, tuple) else None
    return pl.pallas_call(
        kernel,
        out_shape=shapes or jax.ShapeDtypeStruct(shape, dtype),
        in_specs=in_specs,
        out_specs=[VMEM] * len(shapes) if shapes else VMEM,
        scratch_shapes=list(scratch),
        cost_estimate=pl.CostEstimate(flops=flops, bytes_accessed=moved, transcendentals=0),
        compiler_params=pltpu.CompilerParams(vmem_limit_bytes=limit << 20),
    )


def pieces_of(x, axis):
    pieces = [x]
    for step in (1, -1, 2):
        pieces.append(shift(x, axis, step))
    return pieces


def gather_z(block):
    behind = shift(block, LINE, 1)
    ahead = shift(block, LINE, -1)
    near = jnp.stack([behind, block, ahead])
    low = shift(near, LINE, 3)
    high = shift(near[:2], LINE, -3)
    return jnp.concatenate([low, near, high])


def local(tokens, norm_gain, outer_weight, inner_weight, value_weight, conv_taps, out_weight):
    seq, width = tokens.shape[1:]
    depth, columns = outer_weight.shape
    bf16, f32 = jnp.bfloat16, jnp.float32
    half = lax.axis_index("zh")
    z = half * lax.axis_size("zl") + lax.axis_index("zl")
    x, core = lax.axis_index("x"), lax.axis_index("core")
    place = jnp.stack([half, z, x, core, lax.axis_index("y")]).astype(jnp.int32)

    packed = call(
        pack_kernel,
        (4, depth, 3 * columns),
        bf16,
        [ANY] * 3,
        8 * depth * columns,
        30 * depth * columns,
        [pltpu.VMEM((3, depth, columns), bf16), pltpu.SemaphoreType.DMA((3,))],
        limit=60,
    )
    group = exchange(packed(outer_weight, inner_weight, value_weight), "zl")
    other_group = mirror(group)
    near = pieces_of(group, "y")

    norm = call(norm_kernel, (seq, width), bf16, [VMEM] * 2, 8 * seq * width, 4 * seq * width, limit=9)
    normed = norm(tokens.reshape(seq, width), norm_gain.reshape(1, width))
    flops = 3 * seq * width * columns
    weight = pltpu.VMEM((width // 2, 3 * columns), bf16)
    start = call(near_kernel, (seq, 3 * columns), f32, [SMEM] + [VMEM] * 5, flops, 8 * seq * width, [weight])
    total = start(place, normed, *near)
    far = pieces_of(other_group, "y")

    out_rows = gather_z(out_weight)
    taps = lax.dynamic_slice_in_dim(conv_taps, (2 * x + core) * columns, columns, 1)
    gate = call(
        gate_kernel,
        (lax.axis_size("x"), seq, columns),
        bf16,
        [SMEM] + [VMEM] * 7,
        flops,
        8 * seq * width,
        [weight, pltpu.VMEM((8 + seq, columns), f32)],
    )
    rows = pieces_of(out_rows, "y")
    gated = gate(place, normed, *far, total, taps)

    own = exchange(gated, "x")
    other = lax.ppermute(own, "core", [(0, 1), (1, 0)])
    flops = seq * width * columns
    first = call(
        own_kernel,
        ((seq, columns), (width // 2, columns)),
        (f32, bf16),
        [SMEM] + [VMEM] * 5,
        flops,
        4 * seq * width,
        [pltpu.VMEM((width // 2, columns), bf16)],
    )
    total, rest = first(place, own, *rows)
    last = call(other_kernel, (seq, columns), bf16, [VMEM] * 3, flops, 4 * seq * width)
    return last(other, rest, total).reshape(1, seq, columns)


def solution(mesh):
    devices = mesh.devices.reshape(4, 2, 4, 4, 4, 2)
    fine = Mesh(devices, ("rep", "zh", "zl", "y", "x", "core"))
    fs, tp = ("zh", "zl", "y"), ("x", "core")
    in_specs = (
        P(("rep", *fs), None, None),
        P(),
        P(fs, tp),
        P(fs, tp),
        P(fs, tp),
        P(),
        P(fs, tp),
    )
    out_specs = P(("rep", *fs), None, tp)

    return jax.shard_map(local, mesh=fine, in_specs=in_specs, out_specs=out_specs, check_vma=False)
```
